32 devices in a mesh: fs: 16 (over z, y, x), tp: 2 (over core).
Axes of the slice: x: 2, y: 2, z: 4, core: 2. Of those that a mesh axis runs over, the one named last changes fastest.
Arguments:
- inputs: bfloat16 [6144, 2048], P('fs'), may hold values from -6 to 6
- gain: float32 [2048], replicated, may hold values from 0.1 to 1.9
- w_gate: bfloat16 [2048, 2816], P('fs', 'tp'), may hold values from -0.125 to 0.125
- w_up: bfloat16 [2048, 2816], P('fs', 'tp'), may hold values from -0.125 to 0.125
- w_down: bfloat16 [2816, 2048], P('tp', 'fs'), may hold values from -0.109375 to 0.109375
- cotangent: bfloat16 [6144, 2048], P('fs'), may hold values from -6 to 6
Outputs:
- input_gradient: bfloat16 [6144, 2048], P('fs')
- grad_down: float32 [2816, 2048], P('tp', 'fs')
The draws below stay inside these ranges and needn't reach their ends.
All inputs are finite; a program needn't handle non-finite values.
Results may differ from the reference program's by a relative error of at most 0.014.
Values may be sent and summed in bfloat16 or wider, within the bound.
A program may use at most 64 MiB of HBM per device.

```python
import jax
import jax.numpy as jnp
from jax import lax

D = 2048
HID = 2816
TOKENS = 6144
N_TP = 2


def with_spikes(result, own_key, source, target, blocks, factor):
    owner, partner = [(jnp.arange(result.shape[axis_at]) // (result.shape[axis_at] // blocks)).reshape([-1 if axis == axis_at else 1 for axis in range(result.ndim)]) for axis_at in (source, target)]
    chosen = jax.random.permutation(own_key, blocks)[partner]
    strong = (owner == chosen) | (owner == (partner + blocks // 2) % blocks)
    return jnp.where(strong, factor * result, result)


def shard_levels(own_key, shape, split, low, largest):
    level = 1.0
    for dim, shards_of in split:
        heights = jax.random.uniform(jax.random.fold_in(jax.random.fold_in(own_key, 6), dim), (shards_of,), jnp.float32, low / len(split), largest / len(split))
        level = level * jnp.repeat(jnp.exp(heights), shape[dim] // shards_of).reshape((-1,) + (1,) * (len(shape) - 1 - dim))
    return level


def noise(key, dims, spread, reach, shards=(), dtype=jnp.bfloat16):
    result = jax.random.normal(key, dims, jnp.float32) * spread
    if len(shards) > 0:
        result = shard_levels(key, dims, shards, -0.22, 0.18) * result
    return jnp.clip(result, min=-reach, max=reach).astype(dtype)


def gaussian_with(rng, shape, scale, most, cuts, heavy, kind=jnp.bfloat16):
    values = scale * jax.random.normal(rng, shape, jnp.float32)
    if cuts:
        values = values * shard_levels(rng, shape, cuts, -0.22, 0.18)
    return jnp.clip(with_spikes(values, jax.random.fold_in(rng, 3), *heavy), -most, most).astype(kind)


def setup_inputs(seed: int = 0) -> dict:
    seeds = jax.random.split(jax.random.key(seed), 7)
    inputs = noise(seeds[0], (TOKENS, D), 1.0, 6.0, ((0, 16),))
    gain = jnp.clip(1.0 + 0.18 * jax.random.normal(seeds[1], (D,), jnp.float32), 0.1, 1.9)
    w_gate = noise(seeds[2], (D, HID), D ** -0.5, 0.125, ((0, 16), (1, 2)))
    w_up = noise(seeds[3], (D, HID), D ** -0.5, 0.125, ((0, 16), (1, 2)))
    w_down = noise(seeds[4], (HID, D), HID ** -0.5, 0.109375, ((0, 2), (1, 16)))
    cotangent = gaussian_with(seeds[5], (TOKENS, D), 1.0, 6.0, ((0, 16),), (0, 1, 16, 2.0))
    return dict(inputs=inputs, gain=gain, w_gate=w_gate, w_up=w_up, w_down=w_down, cotangent=cotangent)


EPSILON = 1e-06
HALF_STEP = 0.5

def reference(inputs, gain, w_gate, w_up, w_down, cotangent):
    value_entries = inputs.astype(jnp.float32)
    inverse_norm_factor = lax.rsqrt(lax.optimization_barrier(jnp.mean(value_entries * value_entries, axis=-1, keepdims=True)) + EPSILON)
    normalized_input = value_entries * inverse_norm_factor
    normalized_rows = (normalized_input * gain.astype(jnp.float32)).astype(jnp.bfloat16)
    gate_value = jnp.dot(normalized_rows, w_gate, preferred_element_type=jnp.float32)
    up_projection_value = jnp.dot(normalized_rows, w_up, preferred_element_type=jnp.float32)
    sigmoid_gate = jax.nn.sigmoid(gate_value)
    hidden = (gate_value * sigmoid_gate * up_projection_value).astype(jnp.bfloat16)
    d_hidden = HALF_STEP * jnp.dot(cotangent, w_down.T, preferred_element_type=jnp.float32)
    grad_down = HALF_STEP * jnp.dot(hidden.T, cotangent, preferred_element_type=jnp.float32)
    d_gate = (d_hidden * up_projection_value * sigmoid_gate * (1.0 + gate_value * (1.0 - sigmoid_gate))).astype(jnp.bfloat16)
    d_up = (d_hidden * gate_value * sigmoid_gate).astype(jnp.bfloat16)
    block_width = HID // N_TP
    d_normed = jnp.zeros(value_entries.shape, jnp.float32)
    for block in range(N_TP):
        lower = block * block_width
        upper = lower + block_width
        partial_term = jnp.dot(d_gate[:, lower:upper], w_gate[:, lower:upper].T, preferred_element_type=jnp.float32)
        partial_term = partial_term + jnp.dot(d_up[:, lower:upper], w_up[:, lower:upper].T, preferred_element_type=jnp.float32)
        rounded = lax.optimization_barrier(partial_term.astype(jnp.bfloat16))
        d_normed = d_normed + rounded.astype(jnp.float32)
    scaled_hidden = d_normed * gain.astype(jnp.float32)
    input_gradient = inverse_norm_factor * (scaled_hidden - normalized_input * lax.optimization_barrier(jnp.mean(scaled_hidden * normalized_input, axis=-1, keepdims=True)))
    return (input_gradient.astype(jnp.bfloat16), grad_down)
```

```python
import functools

import jax
import jax.numpy as jnp
from jax import lax
from jax.experimental import pallas as pl
from jax.experimental.pallas import tpu as pltpu
from jax.sharding import PartitionSpec as P


EPSILON = 1e-06
HALF_STEP = 0.5


def contract_last(left, right):
    return lax.dot_general(
        left, right, (((1,), (1,)), ((), ())), preferred_element_type=jnp.float32
    )


def shards(inputs, gain, w_gate, w_up, w_down, cotangent):
    value_entries = inputs.astype(jnp.float32)
    inverse_norm_factor = lax.rsqrt(
        jnp.mean(value_entries * value_entries, axis=-1, keepdims=True) + EPSILON
    )
    normalized_input = value_entries * inverse_norm_factor
    normalized_rows = (normalized_input * gain).astype(jnp.bfloat16)
    whole_gate, whole_up = (
        lax.all_gather(w_gate, "fs", axis=0, tiled=True),
        lax.all_gather(w_up, "fs", axis=0, tiled=True),
    )
    gate_value = jnp.dot(normalized_rows, whole_gate, preferred_element_type=jnp.float32)
    up_projection_value = jnp.dot(normalized_rows, whole_up, preferred_element_type=jnp.float32)
    sigmoid_gate = jax.nn.sigmoid(gate_value)
    hidden = (gate_value * sigmoid_gate * up_projection_value).astype(jnp.bfloat16)
    d_hidden = HALF_STEP * contract_last(
        cotangent, lax.all_gather(w_down, "fs", axis=1, tiled=True)
    )
    down_term = HALF_STEP * lax.dot_general(
        hidden, cotangent, (((0,), (0,)), ((), ())), preferred_element_type=jnp.float32
    )
    grad_down = lax.psum_scatter(down_term, "fs", scatter_dimension=1, tiled=True)
    d_gate = (
        d_hidden * up_projection_value * sigmoid_gate * (1.0 + gate_value * (1.0 - sigmoid_gate))
    ).astype(jnp.bfloat16)
    d_up = (d_hidden * gate_value * sigmoid_gate).astype(jnp.bfloat16)
    partial_term = contract_last(d_gate, whole_gate) + contract_last(d_up, whole_up)
    d_normed = lax.psum(partial_term.astype(jnp.bfloat16), "tp").astype(jnp.float32)
    scaled_hidden = d_normed * gain
    input_gradient = inverse_norm_factor * (
        scaled_hidden
        - normalized_input * jnp.mean(scaled_hidden * normalized_input, axis=-1, keepdims=True)
    )
    return (input_gradient.astype(jnp.bfloat16), grad_down)


RING = 4
MESH_ID = pl.DeviceIdType.MESH


def gray(i):
    return i + (i // 2) * (1 - 2 * (i % 2))


def branch_kernel(
    x_ref, n_ref, c_ref, gain_ref, wp_ref, ig_ref, gd_ref,
    tok_n, tok_c, wt, dn, dpart, rs, gd_acc, gd_send, gd_rs, gd_sum,
    s_wa, r_wa, s_wz, r_wz, s_wr, r_wr, s_t, r_t, s_tr, r_tr, s_dd, r_dd,
    s_dn, r_dn, s_rs, r_rs, s_gz, r_gz, s_gp, r_gp, s_ig, r_ig,
):
    fs = lax.axis_index("fs")
    tp = lax.axis_index("tp")
    zi = fs // RING
    pi = fs % RING
    ring = gray(pi)
    rows = n_ref.shape[0]
    half = rows // 2
    hq = wp_ref.shape[2]
    dl = wp_ref.shape[3]
    partner = (fs, 1 - tp)
    mine = pl.ds(pl.multiple_of(tp * half, half), half)
    other = pl.ds(pl.multiple_of((1 - tp) * half, half), half)

    def plane_fs(k, dz=0):
        return ((zi + dz) % 4) * RING + gray((ring + k) % RING)

    def cols(f, width=dl):
        return pl.ds(pl.multiple_of(f * width, width), width)

    def copy(src, dst, ssem, rsem, dev):
        return pltpu.make_async_remote_copy(
            src_ref=src, dst_ref=dst, send_sem=ssem, recv_sem=rsem,
            device_id=dev, device_id_type=MESH_ID,
        )

    pending = []

    def send(src, dst, ssem, rsem, dev):
        c = copy(src, dst, ssem, rsem, dev)
        c.start()
        pending.append(c)

    def arrived(dst, ssem, rsem, dev):
        copy(dst, dst, ssem, rsem, dev).wait_recv()

    barrier = pltpu.get_barrier_semaphore()
    peers = [partner] + [(plane_fs(k), tp) for k in (1, 2, 3)] + [(plane_fs(0, k), tp) for k in (1, 2, 3)]
    for peer in peers:
        pl.semaphore_signal(barrier, inc=1, device_id=peer, device_id_type=MESH_ID)
    pl.semaphore_wait(barrier, len(peers))

    for k in (1, 3, 2):
        f = plane_fs(k)
        send(wp_ref.at[f % RING], wt.at[:, :, cols(fs)], s_wa.at[k - 1], r_wa.at[k - 1], (f, tp))
    for d, dz in ((0, 1), (1, -1)):
        send(wp_ref.at[pi], wt.at[:, :, cols(fs)], s_wz.at[d, 0], r_wz.at[d, 0], (plane_fs(0, dz), tp))
    for t, src, buf in ((0, n_ref, tok_n), (1, c_ref, tok_c)):
        for d, k in ((0, 1), (1, 3)):
            send(src.at[mine, :], buf.at[4 - k, mine, :], s_t.at[t, d], r_t.at[t, d], (plane_fs(k), tp))
    tok_n[0] = n_ref[...]
    tok_c[0] = c_ref[...]
    wt[:, :, cols(fs)] = wp_ref[pi]
    gd_acc[...] = jnp.zeros_like(gd_acc)

    for k in (1, 3, 2):
        s = 4 - k
        place = wt.at[:, :, cols(plane_fs(s))]
        arrived(place, s_wa.at[k - 1], r_wa.at[k - 1], (plane_fs(s), tp))
        for d, dz in ((0, 1), (1, -1)):
            send(place, place, s_wz.at[d, s], r_wz.at[d, s], (plane_fs(0, dz), tp))
    for s in (0, 3, 1, 2):
        for d, dz in ((0, -1), (1, 1)):
            place = wt.at[:, :, cols(plane_fs(s, dz))]
            arrived(place, s_wz.at[d, s], r_wz.at[d, s], (plane_fs(0, dz), tp))
            if s % 2 == d:
                send(place, place, s_wr.at[s], r_wr.at[s], (plane_fs(0, -dz), tp))

    def to_partner(t, buf, slot):
        place = buf.at[slot, mine, :]
        send(place, place, s_dd.at[t, slot], r_dd.at[t, slot], partner)

    for t, buf in ((0, tok_n), (1, tok_c)):
        for d, slot in ((0, 3), (1, 1)):
            place = buf.at[slot, mine, :]
            arrived(place, s_t.at[t, d], r_t.at[t, d], (plane_fs(slot), tp))
            if t == d:
                send(place, buf.at[2, mine, :], s_tr.at[t], r_tr.at[t], (plane_fs(4 - slot), tp))
            to_partner(t, buf, slot)
    for s in (0, 3, 1, 2):
        place = wt.at[:, :, cols(plane_fs(s, 2))]
        arrived(place, s_wr.at[s], r_wr.at[s], (plane_fs(0, 1), tp))

    def exchange(b):
        return copy(dn.at[b, other, :], dpart.at[b], s_dn.at[b], r_dn.at[b], partner)

    def rs_copy(b):
        return copy(dn.at[b, mine, :], rs.at[b], s_rs.at[b], r_rs.at[b], (plane_fs(b), tp))

    def chip_sum(b):
        exchange(b).wait_recv()
        dn[b, mine, :] = (
            dn[b, mine, :].astype(jnp.float32) + dpart[b].astype(jnp.float32)
        ).astype(jnp.bfloat16)

    def last_tokens():
        for t, buf in ((0, tok_n), (1, tok_c)):
            place = buf.at[2, mine, :]
            arrived(place, s_tr.at[t], r_tr.at[t], (plane_fs(1), tp))
            copy(place, place, s_dd.at[t, 2], r_dd.at[t, 2], partner).start()

    def step(i, carry):
        b = gray(i)
        pl.when(i == 3)(last_tokens)

        @pl.when(i > 0)
        def _():
            for t, buf in ((0, tok_n), (1, tok_c)):
                place = buf.at[b, other, :]
                arrived(place, s_dd.at[t, b], r_dd.at[t, b], partner)

        n_b = tok_n[b]
        c_b = tok_c[b]
        gate = contract_last(n_b, wt[0])
        up = contract_last(n_b, wt[1])
        d_hidden = HALF_STEP * contract_last(c_b, wt[2])
        sig = jax.nn.sigmoid(gate)
        act = gate * sig
        hidden = (act * up).astype(jnp.bfloat16)
        d_gate = (d_hidden * up * sig * (1.0 + gate * (1.0 - sig))).astype(jnp.bfloat16)
        d_up = (d_hidden * act).astype(jnp.bfloat16)
        dn[b] = (
            jnp.dot(d_gate, wt[0], preferred_element_type=jnp.float32)
            + jnp.dot(d_up, wt[1], preferred_element_type=jnp.float32)
        ).astype(jnp.bfloat16)
        exchange(b).start()
        gd_acc[...] += lax.dot_general(
            hidden, c_b, (((0,), (0,)), ((), ())), preferred_element_type=jnp.float32
        )

        @pl.when(i >= 2)
        def _():
            last = gray(i - 1)
            chip_sum(last)
            rs_copy(last).start()

        return carry

    lax.fori_loop(0, 4, step, 0)

    gd_send[...] = (HALF_STEP * gd_acc[...]).astype(jnp.bfloat16)
    wide = RING * dl
    gz = [
        copy(gd_send.at[:, cols((zi + k) % 4, wide)], gd_rs.at[k - 1], s_gz.at[k - 1], r_gz.at[k - 1], (plane_fs(0, k), tp))
        for k in (1, 2, 3)
    ]
    for c in (gz[1], gz[0], gz[2]):
        c.start()
    chip_sum(2)
    rs_copy(2).start()
    chip_sum(0)
    for c in gz:
        c.wait_recv()
    total = HALF_STEP * gd_acc[:, cols(zi, wide)]
    for k in range(3):
        total = total + gd_rs[k].astype(jnp.float32)
    for q in range(RING):
        gd_sum[q] = total[:, q * dl:(q + 1) * dl]
    here = pl.ds(pl.multiple_of(pi * hq, hq), hq)
    for k in (1, 3, 2):
        f = plane_fs(k)
        send(gd_sum.at[f % RING], gd_ref.at[here, :], s_gp.at[k - 1], r_gp.at[k - 1], (f, tp))
    gd_ref[here, :] = gd_sum[pi]

    for b in (1, 3, 2):
        rs_copy(b).wait_recv()
    d_normed = dn[0, mine, :].astype(jnp.float32)
    for b in (1, 2, 3):
        d_normed = d_normed + rs[b].astype(jnp.float32)
    values = x_ref[mine, :].astype(jnp.float32)
    inverse = lax.rsqrt(jnp.mean(values * values, axis=-1, keepdims=True) + EPSILON)
    xhat = values * inverse
    scaled = d_normed * gain_ref[...]
    ig_ref[mine, :] = (
        inverse * (scaled - xhat * jnp.mean(scaled * xhat, axis=-1, keepdims=True))
    ).astype(jnp.bfloat16)
    final = copy(ig_ref.at[mine, :], ig_ref.at[mine, :], s_ig, r_ig, partner)
    final.start()

    for k in (1, 3, 2):
        there = pl.ds(pl.multiple_of((plane_fs(4 - k) % RING) * hq, hq), hq)
        arrived(gd_ref.at[there, :], s_gp.at[k - 1], r_gp.at[k - 1], (plane_fs(4 - k), tp))
    arrived(ig_ref.at[other, :], s_ig, r_ig, partner)
    final.wait_send()
    for c in pending + gz:
        c.wait_send()
    for t, buf in ((0, tok_n), (1, tok_c)):
        place = buf.at[2, mine, :]
        copy(place, place, s_dd.at[t, 2], r_dd.at[t, 2], partner).wait_send()
    for b in range(RING):
        exchange(b).wait_send()
        if b:
            rs_copy(b).wait_send()


def fused(inputs, gain, w_gate, w_up, w_down, cotangent):
    rows, d = inputs.shape
    dl, hl = w_gate.shape
    hq = hl // RING
    values = inputs.astype(jnp.float32)
    inverse = lax.rsqrt(jnp.mean(values * values, axis=-1, keepdims=True) + EPSILON)
    normed = (values * inverse * gain).astype(jnp.bfloat16)

    def turned(w):
        return w.reshape(dl, RING, hq).transpose(1, 2, 0)

    packed = jnp.stack([turned(w_gate), turned(w_up), w_down.reshape(RING, hq, dl)], axis=1)
    half = rows // 2
    bf, f32 = jnp.bfloat16, jnp.float32
    dma = pltpu.SemaphoreType.DMA
    vm = pl.BlockSpec(memory_space=pltpu.VMEM)
    pairs = [(3,), (2, 4), (4,), (2, 2), (2,), (2, 4), (4,), (4,), (3,), (3,)]
    sems = []
    for p in pairs:
        sems += [dma(p), dma(p)]
    sems += [dma, dma]
    return pl.pallas_call(
        branch_kernel,
        out_shape=(jax.ShapeDtypeStruct((rows, d), bf), jax.ShapeDtypeStruct((hl, dl), f32)),
        in_specs=[vm] * 5,
        out_specs=(vm, vm),
        scratch_shapes=[
            pltpu.VMEM((RING, rows, d), bf),
            pltpu.VMEM((RING, rows, d), bf),
            pltpu.VMEM((3, hq, d), bf),
            pltpu.VMEM((RING, rows, d), bf),
            pltpu.VMEM((RING, half, d), bf),
            pltpu.VMEM((RING, half, d), bf),
            pltpu.VMEM((hq, d), f32),
            pltpu.VMEM((hq, d), bf),
            pltpu.VMEM((3, hq, RING * dl), bf),
            pltpu.VMEM((RING, hq, dl), f32),
        ] + sems,
        compiler_params=pltpu.CompilerParams(
            collective_id=0, has_side_effects=True, vmem_limit_bytes=67043328
        ),
    )(inputs, normed, cotangent, gain.reshape(1, d), packed)


def fits(mesh, w_gate_shape, rows):
    n_fs, n_tp = mesh.shape["fs"], mesh.shape["tp"]
    dl, hl = w_gate_shape[0] // n_fs, w_gate_shape[1] // n_tp
    return n_fs == RING * RING and n_tp == 2 and dl % 128 == 0 and hl % (16 * RING) == 0 and rows // n_fs % 32 == 0


def solution(mesh):
    in_specs = (P("fs", None), P(), P("fs", "tp"), P("fs", "tp"), P("tp", "fs"), P("fs", None))
    out_specs = (P("fs", None), P("tp", "fs"))

    def run(inputs, gain, w_gate, w_up, w_down, cotangent):
        body = fused if fits(mesh, w_gate.shape, inputs.shape[0]) else shards
        return jax.shard_map(
            body, mesh=mesh, in_specs=in_specs, out_specs=out_specs, check_vma=False
        )(inputs, gain, w_gate, w_up, w_down, cotangent)

    return run
```

```python
import functools

import jax
import jax.numpy as jnp
from jax import lax
from jax.experimental import pallas as pl
from jax.experimental.pallas import tpu as pltpu
from jax.sharding import PartitionSpec as P


EPSILON = 1e-06
HALF_STEP = 0.5


def contract_last(left, right):
    return lax.dot_general(
        left, right, (((1,), (1,)), ((), ())), preferred_element_type=jnp.float32
    )


def shards(inputs, gain, w_gate, w_up, w_down, cotangent):
    value_entries = inputs.astype(jnp.float32)
    inverse_norm_factor = lax.rsqrt(
        jnp.mean(value_entries * value_entries, axis=-1, keepdims=True) + EPSILON
    )
    normalized_input = value_entries * inverse_norm_factor
    normalized_rows = (normalized_input * gain).astype(jnp.bfloat16)
    whole_gate, whole_up = (
        lax.all_gather(w_gate, "fs", axis=0, tiled=True),
        lax.all_gather(w_up, "fs", axis=0, tiled=True),
    )
    gate_value = jnp.dot(normalized_rows, whole_gate, preferred_element_type=jnp.float32)
    up_projection_value = jnp.dot(normalized_rows, whole_up, preferred_element_type=jnp.float32)
    sigmoid_gate = jax.nn.sigmoid(gate_value)
    hidden = (gate_value * sigmoid_gate * up_projection_value).astype(jnp.bfloat16)
    d_hidden = HALF_STEP * contract_last(
        cotangent, lax.all_gather(w_down, "fs", axis=1, tiled=True)
    )
    down_term = HALF_STEP * lax.dot_general(
        hidden, cotangent, (((0,), (0,)), ((), ())), preferred_element_type=jnp.float32
    )
    grad_down = lax.psum_scatter(down_term, "fs", scatter_dimension=1, tiled=True)
    d_gate = (
        d_hidden * up_projection_value * sigmoid_gate * (1.0 + gate_value * (1.0 - sigmoid_gate))
    ).astype(jnp.bfloat16)
    d_up = (d_hidden * gate_value * sigmoid_gate).astype(jnp.bfloat16)
    partial_term = contract_last(d_gate, whole_gate) + contract_last(d_up, whole_up)
    d_normed = lax.psum(partial_term.astype(jnp.bfloat16), "tp").astype(jnp.float32)
    scaled_hidden = d_normed * gain
    input_gradient = inverse_norm_factor * (
        scaled_hidden
        - normalized_input * jnp.mean(scaled_hidden * normalized_input, axis=-1, keepdims=True)
    )
    return (input_gradient.astype(jnp.bfloat16), grad_down)


RING = 4
MESH_ID = pl.DeviceIdType.MESH


def gray(i):
    return i + (i // 2) * (1 - 2 * (i % 2))


def branch_kernel(
    x_ref, n_ref, c_ref, gain_ref, wp_ref, ig_ref, gd_ref,
    tok_n, tok_c, wt, dn, dpart, rs, r_opp, slope, act, gd_acc, gd_send, gd_rs, gd_sum,
    s_wa, r_wa, s_wz, r_wz, s_wr, r_wr, s_t, r_t, s_tr, r_tr, s_dd, r_dd,
    s_dn, r_dn, s_rs, r_rs, s_op, r_op, s_gz, r_gz, s_gp, r_gp, s_ig, r_ig,
):
    fs = lax.axis_index("fs")
    tp = lax.axis_index("tp")
    zi = fs // RING
    pi = fs % RING
    ring = gray(pi)
    rows, width_d = n_ref.shape
    half = rows // 2
    hq = wp_ref.shape[2]
    dl = wp_ref.shape[3]
    partner = (fs, 1 - tp)
    mine = pl.ds(pl.multiple_of(tp * half, half), half)
    other = pl.ds(pl.multiple_of((1 - tp) * half, half), half)
    low, high = pl.ds(0, width_d // 2), pl.ds(width_d // 2, width_d // 2)
    parts = (pl.ds(0, 2), pl.ds(2, 1))

    def plane_fs(k, dz=0):
        return ((zi + dz) % 4) * RING + gray((ring + k) % RING)

    def cols(f, width=dl):
        return pl.ds(pl.multiple_of(f * width, width), width)

    def copy(src, dst, ssem, rsem, dev):
        return pltpu.make_async_remote_copy(
            src_ref=src, dst_ref=dst, send_sem=ssem, recv_sem=rsem,
            device_id=dev, device_id_type=MESH_ID,
        )

    pending = []

    def send(src, dst, ssem, rsem, dev):
        c = copy(src, dst, ssem, rsem, dev)
        c.start()
        pending.append(c)

    def arrived(dst, ssem, rsem, dev):
        copy(dst, dst, ssem, rsem, dev).wait_recv()

    barrier = pltpu.get_barrier_semaphore()
    peers = [partner] + [(plane_fs(k), tp) for k in (1, 2, 3)] + [(plane_fs(0, k), tp) for k in (1, 2, 3)]
    for peer in peers:
        pl.semaphore_signal(barrier, inc=1, device_id=peer, device_id_type=MESH_ID)
    pl.semaphore_wait(barrier, len(peers))

    def weights_plane(p):
        for k in (1, 3, 2):
            f = plane_fs(k)
            send(
                wp_ref.at[f % RING, parts[p]], wt.at[parts[p], :, cols(fs)],
                s_wa.at[p, k - 1], r_wa.at[p, k - 1], (f, tp),
            )

    def weights_own(p):
        for d, dz in ((0, 1), (1, -1)):
            send(
                wp_ref.at[pi, parts[p]], wt.at[parts[p], :, cols(fs)],
                s_wz.at[p, d, 0], r_wz.at[p, d, 0], (plane_fs(0, dz), tp),
            )

    def weights_forward(p):
        for k in (1, 3, 2):
            s = 4 - k
            place = wt.at[parts[p], :, cols(plane_fs(s))]
            arrived(place, s_wa.at[p, k - 1], r_wa.at[p, k - 1], (plane_fs(s), tp))
            for d, dz in ((0, 1), (1, -1)):
                send(place, place, s_wz.at[p, d, s], r_wz.at[p, d, s], (plane_fs(0, dz), tp))

    def relay(p, s, d, dz):
        place = wt.at[parts[p], :, cols(plane_fs(s, dz))]
        return copy(place, place, s_wr.at[p, s], r_wr.at[p, s], (plane_fs(0, -dz), tp))

    def weights_relay(p):
        for s in (0, 3, 1, 2):
            for d, dz in ((0, -1), (1, 1)):
                place = wt.at[parts[p], :, cols(plane_fs(s, dz))]
                arrived(place, s_wz.at[p, d, s], r_wz.at[p, d, s], (plane_fs(0, dz), tp))
                if s % 2 == d:
                    relay(p, s, d, dz).start()

    def weights_last(p):
        for s in (0, 3, 1, 2):
            place = wt.at[parts[p], :, cols(plane_fs(s, 2))]
            arrived(place, s_wr.at[p, s], r_wr.at[p, s], (plane_fs(0, 1), tp))

    def tokens_own(t, src, buf):
        for d, k in ((0, 1), (1, 3)):
            send(src.at[mine, :], buf.at[4 - k, mine, :], s_t.at[t, d], r_t.at[t, d], (plane_fs(k), tp))

    def tokens_relay(t, buf):
        for d, slot in ((0, 3), (1, 1)):
            place = buf.at[slot, mine, :]
            arrived(place, s_t.at[t, d], r_t.at[t, d], (plane_fs(slot), tp))
            if t == d:
                send(place, buf.at[2, mine, :], s_tr.at[t], r_tr.at[t], (plane_fs(4 - slot), tp))
            send(place, place, s_dd.at[t, slot], r_dd.at[t, slot], partner)

    weights_plane(0)
    weights_own(0)
    tokens_own(0, n_ref, tok_n)
    weights_plane(1)
    tokens_own(1, c_ref, tok_c)
    tok_n[0] = n_ref[...]
    tok_c[0] = c_ref[...]
    wt[:, :, cols(fs)] = wp_ref[pi]
    gd_acc[...] = jnp.zeros_like(gd_acc)
    weights_forward(0)
    tokens_relay(0, tok_n)
    weights_relay(0)
    weights_own(1)
    weights_forward(1)
    tokens_relay(1, tok_c)
    weights_last(0)

    def last_tokens():
        weights_relay(1)
        for t, buf in ((0, tok_n), (1, tok_c)):
            place = buf.at[2, mine, :]
            arrived(place, s_tr.at[t], r_tr.at[t], (plane_fs(1), tp))
            copy(place, place, s_dd.at[t, 2], r_dd.at[t, 2], partner).start()

    def forward(i, carry):
        b = gray(i)
        pl.when(i == 3)(last_tokens)

        @pl.when(i > 0)
        def _():
            for t, buf in ((0, tok_n), (1, tok_c)):
                place = buf.at[b, other, :]
                arrived(place, s_dd.at[t, b], r_dd.at[t, b], partner)

        n_b = tok_n[b]
        gate = contract_last(n_b, wt[0])
        up = contract_last(n_b, wt[1])
        sig = jax.nn.sigmoid(gate)
        gated = gate * sig
        hidden = (gated * up).astype(jnp.bfloat16)
        slope[b] = up * sig * (1.0 + gate * (1.0 - sig))
        act[b] = gated
        gd_acc[...] += lax.dot_general(
            hidden, tok_c[b], (((0,), (0,)), ((), ())), preferred_element_type=jnp.float32
        )
        return carry

    lax.fori_loop(0, 4, forward, 0)

    gd_send[...] = (HALF_STEP * gd_acc[...]).astype(jnp.bfloat16)
    wide = RING * dl
    gz = [
        copy(gd_send.at[:, cols((zi + k) % 4, wide)], gd_rs.at[k - 1], s_gz.at[k - 1], r_gz.at[k - 1], (plane_fs(0, k), tp))
        for k in (1, 2, 3)
    ]
    for c in (gz[1], gz[0], gz[2]):
        c.start()
    weights_last(1)

    def exchange(b):
        return copy(dn.at[b, other, :], dpart.at[b], s_dn.at[b], r_dn.at[b], partner)

    def rs_copy(b, part):
        place = (low, high)[part]
        e = 0 if b == 1 else 1
        return copy(dn.at[b, mine, place], rs.at[e, :, place], s_rs.at[e, part], r_rs.at[e, part], (plane_fs(b), tp))

    def opp_copy(e):
        return copy(
            dn.at[2, mine, (low, high)[e]], r_opp.at[e],
            s_op.at[e], r_op.at[e], (plane_fs((1, 3)[e]), tp),
        )

    def chip_sum(b):
        exchange(b).wait_recv()
        dn[b, mine, :] = (
            dn[b, mine, :].astype(jnp.float32) + dpart[b].astype(jnp.float32)
        ).astype(jnp.bfloat16)

    def backward(i, carry):
        b = jnp.where(i == 0, 2, jnp.where(i == 3, 0, 2 * i - 1))
        d_hidden = HALF_STEP * contract_last(tok_c[b], wt[2])
        d_gate = (d_hidden * slope[b]).astype(jnp.bfloat16)
        d_up = (d_hidden * act[b]).astype(jnp.bfloat16)
        dn[b] = (
            jnp.dot(d_gate, wt[0], preferred_element_type=jnp.float32)
            + jnp.dot(d_up, wt[1], preferred_element_type=jnp.float32)
        ).astype(jnp.bfloat16)
        exchange(b).start()

        @pl.when(i == 1)
        def _():
            chip_sum(2)
            opp_copy(0).start()
            opp_copy(1).start()

        @pl.when(i == 2)
        def _():
            chip_sum(1)
            rs_copy(1, 1).start()

        @pl.when(i == 3)
        def _():
            chip_sum(3)
            rs_copy(3, 0).start()

        return carry

    lax.fori_loop(0, 4, backward, 0)

    for e, b, place in ((0, 1, low), (1, 3, high)):
        opp_copy(e).wait_recv()
        dn[b, mine, place] = (
            dn[b, mine, place].astype(jnp.float32) + r_opp[e].astype(jnp.float32)
        ).astype(jnp.bfloat16)
        rs_copy(b, e).start()
    chip_sum(0)
    for c in gz:
        c.wait_recv()
    total = HALF_STEP * gd_acc[:, cols(zi, wide)]
    for k in range(3):
        total = total + gd_rs[k].astype(jnp.float32)
    for q in range(RING):
        gd_sum[q] = total[:, q * dl:(q + 1) * dl]
    here = pl.ds(pl.multiple_of(pi * hq, hq), hq)
    for k in (1, 3, 2):
        f = plane_fs(k)
        send(gd_sum.at[f % RING], gd_ref.at[here, :], s_gp.at[k - 1], r_gp.at[k - 1], (f, tp))
    gd_ref[here, :] = gd_sum[pi]

    for b in (1, 3):
        for part in (0, 1):
            rs_copy(b, part).wait_recv()
    d_normed = dn[0, mine, :].astype(jnp.float32)
    for e in (0, 1):
        d_normed = d_normed + rs[e].astype(jnp.float32)
    values = x_ref[mine, :].astype(jnp.float32)
    inverse = lax.rsqrt(jnp.mean(values * values, axis=-1, keepdims=True) + EPSILON)
    xhat = values * inverse
    scaled = d_normed * gain_ref[...]
    ig_ref[mine, :] = (
        inverse * (scaled - xhat * jnp.mean(scaled * xhat, axis=-1, keepdims=True))
    ).astype(jnp.bfloat16)
    final = copy(ig_ref.at[mine, :], ig_ref.at[mine, :], s_ig, r_ig, partner)
    final.start()

    for k in (1, 3, 2):
        there = pl.ds(pl.multiple_of((plane_fs(4 - k) % RING) * hq, hq), hq)
        arrived(gd_ref.at[there, :], s_gp.at[k - 1], r_gp.at[k - 1], (plane_fs(4 - k), tp))
    arrived(ig_ref.at[other, :], s_ig, r_ig, partner)
    final.wait_send()
    for c in pending + gz:
        c.wait_send()
    for p in (0, 1):
        for s in range(RING):
            relay(p, s, s % 2, (-1, 1)[s % 2]).wait_send()
    for t, buf in ((0, tok_n), (1, tok_c)):
        place = buf.at[2, mine, :]
        copy(place, place, s_dd.at[t, 2], r_dd.at[t, 2], partner).wait_send()
    for b in range(RING):
        exchange(b).wait_send()
    for e in (0, 1):
        opp_copy(e).wait_send()
        for part in (0, 1):
            rs_copy((1, 3)[e], part).wait_send()


def fused(inputs, gain, w_gate, w_up, w_down, cotangent):
    rows, d = inputs.shape
    dl, hl = w_gate.shape
    hq = hl // RING
    values = inputs.astype(jnp.float32)
    inverse = lax.rsqrt(jnp.mean(values * values, axis=-1, keepdims=True) + EPSILON)
    normed = (values * inverse * gain).astype(jnp.bfloat16)

    def turned(w):
        return w.reshape(dl, RING, hq).transpose(1, 2, 0)

    packed = jnp.stack([turned(w_gate), turned(w_up), w_down.reshape(RING, hq, dl)], axis=1)
    half = rows // 2
    bf, f32 = jnp.bfloat16, jnp.float32
    dma = pltpu.SemaphoreType.DMA
    vm = pl.BlockSpec(memory_space=pltpu.VMEM)
    pairs = [(2, 3), (2, 2, 4), (2, 4), (2, 2), (2,), (2, 4), (4,), (2, 2), (2,), (3,), (3,)]
    sems = []
    for p in pairs:
        sems += [dma(p), dma(p)]
    sems += [dma, dma]
    return pl.pallas_call(
        branch_kernel,
        out_shape=(jax.ShapeDtypeStruct((rows, d), bf), jax.ShapeDtypeStruct((hl, dl), f32)),
        in_specs=[vm] * 5,
        out_specs=(vm, vm),
        scratch_shapes=[
            pltpu.VMEM((RING, rows, d), bf),
            pltpu.VMEM((RING, rows, d), bf),
            pltpu.VMEM((3, hq, d), bf),
            pltpu.VMEM((RING, rows, d), bf),
            pltpu.VMEM((RING, half, d), bf),
            pltpu.VMEM((2, half, d), bf),
            pltpu.VMEM((2, half, d // 2), bf),
            pltpu.VMEM((RING, rows, hq), f32),
            pltpu.VMEM((RING, rows, hq), f32),
            pltpu.VMEM((hq, d), f32),
            pltpu.VMEM((hq, d), bf),
            pltpu.VMEM((3, hq, RING * dl), bf),
            pltpu.VMEM((RING, hq, dl), f32),
        ] + sems,
        compiler_params=pltpu.CompilerParams(
            collective_id=0, has_side_effects=True, vmem_limit_bytes=67043328
        ),
    )(inputs, normed, cotangent, gain.reshape(1, d), packed)


def fits(mesh, w_gate_shape, rows):
    n_fs, n_tp = mesh.shape["fs"], mesh.shape["tp"]
    dl, hl = w_gate_shape[0] // n_fs, w_gate_shape[1] // n_tp
    return n_fs == RING * RING and n_tp == 2 and dl % 128 == 0 and hl % (16 * RING) == 0 and rows // n_fs % 32 == 0


def solution(mesh):
    in_specs = (P("fs", None), P(), P("fs", "tp"), P("fs", "tp"), P("tp", "fs"), P("fs", None))
    out_specs = (P("fs", None), P("tp", "fs"))

    def run(inputs, gain, w_gate, w_up, w_down, cotangent):
        body = fused if fits(mesh, w_gate.shape, inputs.shape[0]) else shards
        return jax.shard_map(
            body, mesh=mesh, in_specs=in_specs, out_specs=out_specs, check_vma=False
        )(inputs, gain, w_gate, w_up, w_down, cotangent)

    return run
```
